32 devices in a mesh: grp: 2 (over y), sp: 4 (over z), tp: 4 (over x, core).
Axes of the slice: x: 2, y: 2, z: 4, core: 2. Of those that a mesh axis runs over, the one named last changes fastest.
Arguments:
- target: bfloat16 [1024, 2048], P(('grp', 'sp', 'tp')), parts along dimension 0, may hold values from -60 to 60
- source: bfloat16 [8192, 2048], P(('grp', 'sp', 'tp')), parts along dimension 0, may hold values from -120 to 120
- w_query: bfloat16 [2, 2048, 2048], P(None, None, 'tp'), may hold values from -0.176776695 to 0.176776695
- w_key: bfloat16 [2, 2048, 2048], P(None, None, 'tp'), may hold values from -0.176776695 to 0.176776695
- w_value: bfloat16 [2, 2048, 2048], P(None, None, 'tp'), may hold values from -0.125 to 0.125
- w_out: bfloat16 [2, 2048, 2048], P(None, 'tp'), may hold values from -0.125 to 0.125
- gains: float32 [2, 2, 2048], replicated, may hold values from 0.1 to 1.9
Outputs:
- mixed: bfloat16 [1024, 2048], P(('grp', 'sp', 'tp')), parts along dimension 0
The draws below stay inside these ranges and needn't reach their ends.
There are 2 independent parts, one for each index of `grp`. The reference program is written for one: setup_inputs(seed, part) draws one part's arguments, and reference() takes and returns one part's arrays. A program takes and returns all parts, laid end to end along the dimension named above; an argument that names none is the same for every part. Nothing has to cross between parts.
All inputs are finite; a program needn't handle non-finite values.
Results may differ from the reference program's by a relative error of at most 0.025.
Values may be sent and summed in bfloat16 or wider, within the bound.
A program may use at most 128 MiB of HBM per device.

```python
import jax
import jax.numpy as jnp
from jax import lax

D = 2048
HEADS = 16
HEAD = 128
LAYERS = 2
TGT = 512
SRC = 4096
N_TP = 4


def draw_target(key, part):
    base = jnp.clip(jax.random.normal(jax.random.fold_in(key, 11), (TGT, D), jnp.float32), -6.0, 6.0)
    return base.astype(jnp.bfloat16)


def draw_source(key, part):
    base = jnp.clip(jax.random.normal(jax.random.fold_in(key, 21), (SRC, D), jnp.float32), -6.0, 6.0)
    return base.astype(jnp.bfloat16)


def draw_w_query(key, part):
    shared = jnp.clip(jax.random.normal(jax.random.fold_in(key, 31), (LAYERS, D, D), jnp.float32), -6.0, 6.0)
    return (shared * D ** (-0.5)).astype(jnp.bfloat16)


def draw_w_key(key, part):
    fresh = jnp.clip(jax.random.normal(jax.random.fold_in(key, 32), (LAYERS, D, D), jnp.float32), -6.0, 6.0)
    return (fresh * D ** (-0.5)).astype(jnp.bfloat16)


def steps_of(key, extent, pieces, smallest, top_value):
    level = 1.0
    for dim, shards_of in pieces:
        steps = jax.random.uniform(jax.random.fold_in(jax.random.fold_in(key, 6), dim), (shards_of,), jnp.float32, smallest / len(pieces), top_value / len(pieces))
        level = level * jnp.repeat(jnp.exp(steps), extent[dim] // shards_of).reshape((-1,) + (1,) * (len(extent) - 1 - dim))
    return level


def bell_draw(rng, extent, width, bound, cuts=(), held_as=jnp.bfloat16):
    result = jax.random.normal(rng, extent, jnp.float32) * width
    if len(cuts) > 0:
        result = steps_of(rng, extent, cuts, -0.22, 0.18) * result
    return jnp.clip(result, min=-bound, max=bound).astype(held_as)


def setup_inputs(seed: int = 0, part: int = 0) -> dict:
    key_list = jax.random.split(jax.random.key(seed), 8)
    part_splits = jax.random.split(jax.random.fold_in(key_list[7], part), 8)
    return {
        "target": draw_target(jax.random.fold_in(jax.random.fold_in(key_list[7], part), 71), part),
        "source": draw_source(jax.random.fold_in(jax.random.fold_in(key_list[7], part), 71), part),
        "w_query": draw_w_query(jax.random.fold_in(key_list[7], 71), part),
        "w_key": draw_w_key(jax.random.fold_in(key_list[7], 71), part),
        "w_value": bell_draw(key_list[4], (LAYERS, D, D), D ** -0.5, 0.125, ((2, 4),)),
        "w_out": bell_draw(key_list[5], (LAYERS, D, D), D ** -0.5, 0.125, ((1, 4),)),
        "gains": jnp.clip(1.0 + 0.18 * jax.random.normal(key_list[6], (LAYERS, 2, D), jnp.float32), 0.1, 1.9),
    }


EPS = 1e-06

def normalize(row_block, gain_row):
    return row_block * lax.rsqrt(lax.optimization_barrier(jnp.mean(row_block * row_block, axis=-1, keepdims=True)) + EPS) * gain_row.astype(jnp.float32)

def attend_head(query_cols, key_cols, value_cols):
    scores = jnp.dot(query_cols, key_cols.T, preferred_element_type=jnp.float32) * HEAD ** (-0.5)
    row_peak = lax.optimization_barrier(jnp.max(scores, axis=1, keepdims=True))
    weights = jnp.exp(scores - row_peak)
    row_total = lax.optimization_barrier(jnp.sum(weights, axis=1, keepdims=True))
    summed = jnp.dot(weights.astype(jnp.bfloat16), value_cols, preferred_element_type=jnp.float32)
    return (summed / row_total).astype(jnp.bfloat16)

def reference(target, source, w_query, w_key, w_value, w_out, gains):
    stream = target.astype(jnp.float32)
    group_width = D // N_TP
    for layer_index in range(LAYERS):
        keys = jnp.dot(source, w_key[layer_index], preferred_element_type=jnp.float32).astype(jnp.bfloat16)
        values = jnp.dot(source, w_value[layer_index], preferred_element_type=jnp.float32).astype(jnp.bfloat16)
        normed = normalize(stream, gains[layer_index, 0]).astype(jnp.bfloat16)
        queries = jnp.dot(normed, w_query[layer_index], preferred_element_type=jnp.float32).astype(jnp.bfloat16)

        def one_head(head_index):
            offset = (head_index * HEAD).astype(jnp.int32)
            return attend_head(lax.dynamic_slice_in_dim(queries, offset, HEAD, 1), lax.dynamic_slice_in_dim(keys, offset, HEAD, 1), lax.dynamic_slice_in_dim(values, offset, HEAD, 1))
        heads_out = lax.map(one_head, jnp.arange(HEADS, dtype=jnp.int32))
        attended = jnp.transpose(heads_out, (1, 0, 2)).reshape(TGT, D)
        out_weight = w_out[layer_index]

        def add_group(running, group_index):
            offset = (group_index * group_width).astype(jnp.int32)
            partial_value = jnp.dot(lax.dynamic_slice_in_dim(attended, offset, group_width, 1), lax.dynamic_slice_in_dim(out_weight, offset, group_width, 0), preferred_element_type=jnp.float32)
            rounded = lax.optimization_barrier(partial_value.astype(jnp.bfloat16))
            return (running + rounded.astype(jnp.float32), None)
        projected, _ = lax.scan(add_group, jnp.zeros((TGT, D), jnp.float32), jnp.arange(N_TP, dtype=jnp.int32))
        stream = stream + normalize(projected, gains[layer_index, 1])
    return stream.astype(jnp.bfloat16)
```

```python
import functools
import math

import jax
import jax.numpy as jnp
from jax import lax
from jax.experimental import pallas as pl
from jax.experimental.pallas import tpu as pltpu
from jax.sharding import PartitionSpec as P

HEAD = 128
CORES = 2


EPS = 1e-06
MESH = pl.DeviceIdType.MESH
F32 = jnp.float32
BF16 = jnp.bfloat16


def normalize(row_block, gain_row):
    return (
        row_block
        * lax.rsqrt(jnp.mean(row_block * row_block, axis=-1, keepdims=True) + EPS)
        * gain_row
    )


def fused_kernel(
    nx, sp, depth,
    target, source, w_query, w_key, w_value, w_out, gains, out,
    tbuf, sbuf, wq, wk, wv, wo, keys, values, stream, normed, qbuf,
    osend, orecv, ssend, srecv, attended, pbuf, half_in, chip_sum, fin,
    local_sem, weight_sem, t_send, t_recv, t_fsend, s_psend, s_send, s_recv, s_fsend,
    q_send, q_recv, o_send, o_recv, e_send, e_recv,
    h_send, h_recv, c_send, c_psend, c_fsend, c_recv, c_frecv, f_send, f_recv,
):
    s = lax.axis_index("sp")
    t = lax.axis_index("tp")
    x = t // CORES
    c = t % CORES
    partner_c = 1 - c
    partner = {"tp": x * CORES + partner_c}
    units = sbuf.shape[0]
    half = sbuf.shape[2]
    width = sbuf.shape[3]
    rows = 2 * half
    local_width = wk.shape[2]
    heads = local_width // HEAD
    tp = nx * CORES
    trows = tbuf.shape[1]
    score_scale = HEAD ** (-0.5) * math.log2(math.e)

    def chip(step):
        return lax.rem(x + step, nx)

    def peer(step):
        return {"tp": chip(step) * CORES + c}

    def remote(src, dst, send_sem, recv_sem, device):
        return pltpu.make_async_remote_copy(
            src_ref=src, dst_ref=dst, send_sem=send_sem, recv_sem=recv_sem,
            device_id=device, device_id_type=MESH,
        )

    def arrived(dst, recv_sem):
        remote(dst, dst, t_send.at[0], recv_sem, partner).wait_recv()

    own_target = pltpu.make_async_copy(target, tbuf.at[t], local_sem.at[0])
    own_source = [
        pltpu.make_async_copy(
            source.at[pl.ds(part * half, half)], sbuf.at[0, part], local_sem.at[1 + part])
        for part in range(2)
    ]

    def load(kind, level):
        pair = ((w_query, wq), (w_key, wk), (w_value, wv), (w_out, wo))[kind]
        return pltpu.make_async_copy(
            pair[0].at[level], pair[1].at[level], weight_sem.at[kind, level])

    own_target.start()
    for copy in own_source:
        copy.start()
    load(1, 0).start()
    load(2, 0).start()

    barrier = pltpu.get_barrier_semaphore()
    pl.semaphore_signal(barrier, inc=1, device_id=partner, device_id_type=MESH)
    for step in range(1, nx):
        pl.semaphore_signal(barrier, inc=1, device_id=peer(step), device_id_type=MESH)
    for step in range(1, sp):
        pl.semaphore_signal(
            barrier, inc=1, device_id={"sp": lax.rem(s + step, sp)}, device_id_type=MESH)
    pl.semaphore_wait(barrier, 1 + (nx - 1) + (sp - 1))

    sends = []

    def go(copy):
        copy.start()
        sends.append(copy)

    for step in range(1, nx):
        go(remote(target, tbuf.at[t], t_send.at[step], t_recv.at[t], peer(step)))
    go(remote(target, tbuf.at[t], t_send.at[0], t_recv.at[t], partner))
    for part in range(2):
        block = source.at[pl.ds(part * half, half)]
        for step in range(1, nx):
            unit = 2 * (nx - step) + part
            go(remote(block, sbuf.at[unit, 0], s_send.at[step, part], s_recv.at[unit, 0], peer(step)))
        go(remote(block, sbuf.at[1, part], s_psend.at[part], s_recv.at[1, part], partner))

    def project(index):
        unit = index // depth
        level = index % depth
        block = sbuf[unit].reshape(rows, width)
        start = pl.multiple_of(unit * rows, rows)
        k = jnp.dot(block, wk[level], preferred_element_type=F32)
        keys[level, pl.ds(start, rows), :] = k.astype(BF16)
        v = jnp.dot(block, wv[level], preferred_element_type=F32)
        values[level, :, pl.ds(start, rows)] = v.T.astype(BF16)

    def make_queries(level):
        q = jnp.dot(normed[...].reshape(tp * trows, width), wq[level], preferred_element_type=F32)
        qbuf[level, s] = q.astype(BF16)
        for step in range(1, sp):
            dest = lax.rem(s + step, sp)
            remote(qbuf.at[level, s], qbuf.at[level, s], q_send.at[level, step],
                   q_recv.at[level, s], {"sp": dest}).start()

    def first_queries():
        own_target.wait()
        for step in range(1, nx):
            slot = chip(step) * CORES + c
            arrived(tbuf.at[slot], t_recv.at[slot])
            remote(tbuf.at[slot], tbuf.at[slot], t_fsend.at[step], t_recv.at[slot], partner).start()
        for step in range(nx):
            slot = chip(step) * CORES + partner_c
            arrived(tbuf.at[slot], t_recv.at[slot])

        @pl.loop(0, tp)
        def _(block):
            value = tbuf[block].astype(F32)
            stream[block] = value
            normed[block] = normalize(value, gains[0, 0:1, :]).astype(BF16)

        load(0, 0).wait()
        make_queries(0)

    @pl.loop(0, units * depth - (depth - 1))
    def _(index):
        unit = index // depth
        level = index % depth

        @pl.when(index == 0)
        def _():
            for copy in own_source:
                copy.wait()
            load(1, 0).wait()
            load(2, 0).wait()
            load(0, 0).start()
            for later in range(1, depth):
                load(1, later).start()
                load(2, later).start()
            load(3, 0).start()
            for later in range(1, depth):
                load(0, later).start()
                load(3, later).start()

        for later in range(1, depth):
            @pl.when(index == later)
            def _():
                load(1, later).wait()
                load(2, later).wait()

        @pl.when(index == depth)
        def _():
            first_queries()
            for part in range(2):
                arrived(sbuf.at[1, part], s_recv.at[1, part])

        @pl.when(jnp.logical_and(unit >= 2, level == 0))
        def _():
            arrived(sbuf.at[unit, 0], s_recv.at[unit, 0])
            remote(sbuf.at[unit, 0], sbuf.at[unit, 1], s_fsend.at[unit],
                   s_recv.at[unit, 1], partner).start()
            arrived(sbuf.at[unit, 1], s_recv.at[unit, 1])

        project(index)

    both = jnp.minimum(s, sp - 1 - s)

    def near(i):
        side = jnp.where(i % 2 == 1, s - (i + 1) // 2, s + i // 2)
        rest = jnp.where(s < sp - 1 - s, i, sp - 1 - i)
        return jnp.where(i <= 2 * both, side, rest)

    for layer in range(depth):
        last = layer == depth - 1

        @pl.loop(0, sp)
        def _(i):
            j = near(i)

            @pl.when(j != s)
            def _():
                arrived(qbuf.at[layer, j], q_recv.at[layer, j])

            q = qbuf[layer, j]
            peaks, totals = [], []
            for h in range(heads):
                cols = slice(h * HEAD, (h + 1) * HEAD)
                scores = lax.dot_general(
                    keys[layer, :, cols], q[:, cols], (((1,), (1,)), ((), ())),
                    preferred_element_type=F32)
                peak = jnp.max(scores, axis=0, keepdims=True) * score_scale
                weights = jnp.exp2(scores * score_scale - peak)
                totals.append(jnp.sum(weights, axis=0, keepdims=True))
                peaks.append(peak)
                o = jnp.dot(values[layer, cols, :], weights.astype(BF16), preferred_element_type=F32)
                osend[layer, j, cols, :] = o.astype(BF16)
            ssend[layer, j] = jnp.concatenate(peaks + totals, axis=0)

            @pl.when(j != s)
            def _():
                remote(osend.at[layer, j], orecv.at[layer, s], o_send.at[layer, j],
                       o_recv.at[layer, s], {"sp": j}).start()
                remote(ssend.at[layer, j], srecv.at[layer, s], e_send.at[layer, j],
                       e_recv.at[layer, s], {"sp": j}).start()

            @pl.when(j == s)
            def _():
                orecv[layer, s] = osend[layer, s]
                srecv[layer, s] = ssend[layer, s]

        if layer == 0:
            @pl.loop(units * depth - (depth - 1), units * depth)
            def _(index):
                project(index)
        load(3, layer).wait()

        for step in range(1, sp):
            j = lax.rem(s + step, sp)
            arrived(orecv.at[layer, j], o_recv.at[layer, j])
            arrived(srecv.at[layer, j], e_recv.at[layer, j])
        peaks = [srecv[layer, j, 0:heads, :] for j in range(sp)]
        top = functools.reduce(jnp.maximum, peaks)
        share = [jnp.exp2(p - top) for p in peaks]
        total = sum(share[j] * srecv[layer, j, heads:2 * heads, :] for j in range(sp))
        share = [one / total for one in share]
        for h in range(heads):
            cols = slice(h * HEAD, (h + 1) * HEAD)
            mixed = sum(share[j][h:h + 1, :] * orecv[layer, j, cols, :].astype(F32) for j in range(sp))
            attended[:, cols] = mixed.T.astype(BF16)

        tile = min(512, width)
        for n in range(width // tile):
            cols = slice(n * tile, (n + 1) * tile)
            part = jnp.dot(attended[...], wo[layer, :, cols], preferred_element_type=F32)
            pbuf[layer, :, :, :, cols] = part.astype(BF16).reshape(nx, CORES, trows, tile)

        go(remote(pbuf.at[layer, :, partner_c], half_in.at[layer], h_send.at[layer],
                  h_recv.at[layer], partner))
        arrived(half_in.at[layer], h_recv.at[layer])
        if not last:
            for b in range(nx):
                both_cores = pbuf[layer, b, c].astype(F32) + half_in[layer, b].astype(F32)
                chip_sum[layer, x, c, b] = both_cores.astype(BF16)
            own = chip_sum.at[layer, x, c]
            for step in range(1, nx):
                go(remote(own, own, c_send.at[layer, step], c_recv.at[layer, x], peer(step)))
            go(remote(own, own, c_psend.at[layer], c_frecv.at[layer, x], partner))
            for step in range(1, nx):
                other = chip_sum.at[layer, chip(step), c]
                arrived(other, c_recv.at[layer, chip(step)])
                go(remote(other, other, c_fsend.at[layer, step], c_frecv.at[layer, chip(step)], partner))
            for step in range(nx):
                arrived(chip_sum.at[layer, chip(step), partner_c], c_frecv.at[layer, chip(step)])
            load(0, layer + 1).wait()

            @pl.loop(0, tp)
            def _(block):
                projected = sum(
                    chip_sum[layer, a, block % CORES, block // CORES].astype(F32) for a in range(nx))
                value = stream[block] + normalize(projected, gains[layer, 1:2, :])
                stream[block] = value
                normed[block] = normalize(value, gains[layer + 1, 0:1, :]).astype(BF16)

            make_queries(layer + 1)
        else:
            for step in range(1, nx):
                b = chip(step)
                both_cores = pbuf[layer, b, c].astype(F32) + half_in[layer, b].astype(F32)
                fin[0, b] = both_cores.astype(BF16)
                go(remote(fin.at[0, b], fin.at[1, x], f_send.at[step], f_recv.at[x], peer(step)))
            projected = pbuf[layer, x, c].astype(F32) + half_in[layer, x].astype(F32)
            for step in range(1, nx):
                b = chip(step)
                arrived(fin.at[1, b], f_recv.at[b])
                projected = projected + fin[1, b].astype(F32)
            value = stream[t] + normalize(projected, gains[layer, 1:2, :])
            out[...] = value.astype(out.dtype)

    for copy in sends:
        copy.wait_send()
    for step in range(1, nx):
        slot = chip(step) * CORES + c
        remote(tbuf.at[slot], tbuf.at[slot], t_fsend.at[step], t_recv.at[slot], partner).wait_send()
    for unit in range(2, units):
        remote(sbuf.at[unit, 0], sbuf.at[unit, 1], s_fsend.at[unit],
               s_recv.at[unit, 1], partner).wait_send()
    for layer in range(depth):
        for step in range(1, sp):
            j = lax.rem(s + step, sp)
            remote(qbuf.at[layer, s], qbuf.at[layer, s], q_send.at[layer, step],
                   q_recv.at[layer, s], {"sp": j}).wait_send()
            remote(osend.at[layer, j], orecv.at[layer, s], o_send.at[layer, j],
                   o_recv.at[layer, s], {"sp": j}).wait_send()
            remote(ssend.at[layer, j], srecv.at[layer, s], e_send.at[layer, j],
                   e_recv.at[layer, s], {"sp": j}).wait_send()


def fused_body(nx, sp, target, source, w_query, w_key, w_value, w_out, gains):
    depth, width, local_width = w_query.shape
    trows, rows = target.shape[0], source.shape[0]
    tp = nx * CORES
    block_rows = tp * trows
    heads = local_width // HEAD
    units = 2 * nx
    vmem = pltpu.VMEM
    dma = pltpu.SemaphoreType.DMA
    anywhere = pl.BlockSpec(memory_space=pl.ANY)
    whole = pl.BlockSpec(memory_space=pltpu.VMEM)
    return pl.pallas_call(
        functools.partial(fused_kernel, nx, sp, depth),
        out_shape=jax.ShapeDtypeStruct((trows, width), BF16),
        in_specs=[anywhere] * 6 + [whole],
        out_specs=whole,
        scratch_shapes=[
            vmem((tp, trows, width), BF16),
            vmem((units, 2, rows // 2, width), BF16),
            vmem(w_query.shape, BF16),
            vmem(w_key.shape, BF16),
            vmem(w_value.shape, BF16),
            vmem(w_out.shape, BF16),
            vmem((depth, units * rows, local_width), BF16),
            vmem((depth, local_width, units * rows), BF16),
            vmem((tp, trows, width), F32),
            vmem((tp, trows, width), BF16),
            vmem((depth, sp, block_rows, local_width), BF16),
            vmem((depth, sp, local_width, block_rows), BF16),
            vmem((depth, sp, local_width, block_rows), BF16),
            vmem((depth, sp, 2 * heads, block_rows), F32),
            vmem((depth, sp, 2 * heads, block_rows), F32),
            vmem((block_rows, local_width), BF16),
            vmem((depth, nx, CORES, trows, width), BF16),
            vmem((depth, nx, trows, width), BF16),
            vmem((depth, nx, CORES, nx, trows, width), BF16),
            vmem((2, nx, trows, width), BF16),
            dma((3,)), dma((4, depth)),
            dma((nx,)), dma((tp,)), dma((nx,)),
            dma((2,)), dma((nx, 2)), dma((units, 2)), dma((units,)),
            dma((depth, sp)), dma((depth, sp)),
            dma((depth, sp)), dma((depth, sp)), dma((depth, sp)), dma((depth, sp)),
            dma((depth,)), dma((depth,)),
            dma((depth, nx)), dma((depth,)), dma((depth, nx)), dma((depth, nx)), dma((depth, nx)),
            dma((nx,)), dma((nx,)),
        ],
        compiler_params=pltpu.CompilerParams(
            collective_id=0, has_side_effects=True, vmem_limit_bytes=60 * 1024 * 1024),
    )(target, source, w_query, w_key, w_value, w_out, gains)


def split_heads(row_block):
    return row_block.reshape(row_block.shape[0], row_block.shape[1] // HEAD, HEAD)


def body(target, source, w_query, w_key, w_value, w_out, gains):
    local_width = w_query.shape[2]
    score_scale = HEAD ** (-0.5)
    depth = w_query.shape[0]
    project_shard_part = lax.all_gather(source, "tp", axis=0, tiled=True)
    layer_parts = [
        jnp.stack(
            [
                jnp.dot(project_shard_part, w_key[level], preferred_element_type=jnp.float32),
                jnp.dot(project_shard_part, w_value[level], preferred_element_type=jnp.float32),
            ]
        )
        for level in range(depth)
    ]
    projected_source = jnp.stack(layer_parts).astype(jnp.bfloat16)
    stream = target.astype(jnp.float32)
    for layer_index in range(depth):
        normed = normalize(stream, gains[layer_index, 0]).astype(jnp.bfloat16)
        query_weight = w_query[layer_index]
        queries = jnp.dot(
            lax.all_gather(normed, "tp", axis=0, tiled=True),
            query_weight,
            preferred_element_type=jnp.float32,
        ).astype(jnp.bfloat16)
        row_count = queries.shape[0]
        keys_here = projected_source[layer_index, 0]
        values_here = projected_source[layer_index, 1]
        every_query = lax.all_gather(queries, "sp", axis=0, tiled=True)
        scores = (
            jnp.einsum(
                "qhd,khd->hqk",
                split_heads(every_query),
                split_heads(keys_here),
                preferred_element_type=jnp.float32,
            )
            * score_scale
        )
        row_peak = lax.pmax(jnp.max(scores, axis=2), "sp")
        weights = jnp.exp(scores - row_peak[:, :, None])
        local_summed = jnp.einsum(
            "hqk,khd->hqd",
            weights.astype(jnp.bfloat16),
            split_heads(values_here),
            preferred_element_type=jnp.float32,
        )
        summed, row_total = (
            lax.psum_scatter(
                local_summed.astype(jnp.bfloat16), "sp", scatter_dimension=1, tiled=True
            ).astype(jnp.float32),
            lax.psum_scatter(
                jnp.sum(weights, axis=2).astype(jnp.bfloat16), "sp", scatter_dimension=1, tiled=True
            ).astype(jnp.float32),
        )
        heads_out = summed / row_total[:, :, None]
        attended = (
            jnp.transpose(heads_out, (1, 0, 2)).reshape(row_count, local_width).astype(jnp.bfloat16)
        )
        out_weight = w_out[layer_index]
        projected = lax.psum_scatter(
            jnp.dot(attended, out_weight, preferred_element_type=jnp.float32).astype(jnp.bfloat16),
            "tp",
            scatter_dimension=0,
            tiled=True,
        ).astype(jnp.float32)
        stream = stream + normalize(projected, gains[layer_index, 1])
    return stream.astype(jnp.bfloat16)


def solution(mesh):
    in_specs = (
        P(("grp", "sp", "tp"), None),
        P(("grp", "sp", "tp"), None),
        P(None, None, "tp"),
        P(None, None, "tp"),
        P(None, None, "tp"),
        P(None, "tp", None),
        P(),
    )
    out_specs = P(("grp", "sp", "tp"), None)
    sp, tp = mesh.shape["sp"], mesh.shape["tp"]

    def run(target, source, w_query, w_key, w_value, w_out, gains):
        trows, rows, local_width = target.shape[0], source.shape[0], w_query.shape[2]
        tiles = (trows % 16 == 0 and (tp * trows) % 128 == 0 and rows % 128 == 0
                 and local_width % (4 * HEAD) == 0 and tp % CORES == 0)
        form = functools.partial(fused_body, tp // CORES, sp) if tiles else body
        return form(target, source, w_query, w_key, w_value, w_out, gains)

    return jax.shard_map(run, mesh=mesh, in_specs=in_specs, out_specs=out_specs, check_vma=False)
```

```python
import functools
import math

import jax
import jax.numpy as jnp
from jax import lax
from jax.experimental import pallas as pl
from jax.experimental.pallas import tpu as pltpu
from jax.sharding import PartitionSpec as P

HEAD = 128
CORES = 2


EPS = 1e-06
MESH = pl.DeviceIdType.MESH
F32 = jnp.float32
BF16 = jnp.bfloat16


def normalize(row_block, gain_row):
    return (
        row_block
        * lax.rsqrt(jnp.mean(row_block * row_block, axis=-1, keepdims=True) + EPS)
        * gain_row
    )


def fused_kernel(
    nx, sp, depth,
    target, source, w_query, w_key, w_value, w_out, gains, out,
    tbuf, sbuf, wq, wk, wv, wo, keys, values, stream, normed, qbuf,
    osend, orecv, ssend, srecv, attended, pbuf, half_in, chip_sum, fin,
    local_sem, weight_sem, t_send, t_recv, t_fsend, s_psend, s_send, s_recv, s_fsend,
    q_send, q_recv, o_send, o_recv, e_send, e_recv,
    h_send, h_recv, c_send, c_psend, c_fsend, c_recv, c_frecv, f_send, f_recv,
):
    s = lax.axis_index("sp")
    t = lax.axis_index("tp")
    x = t // CORES
    c = t % CORES
    partner_c = 1 - c
    partner = {"tp": x * CORES + partner_c}
    units = sbuf.shape[0]
    half = sbuf.shape[2]
    width = sbuf.shape[3]
    rows = 2 * half
    local_width = wk.shape[2]
    heads = local_width // HEAD
    tp = nx * CORES
    trows = tbuf.shape[1]
    score_scale = HEAD ** (-0.5) * math.log2(math.e)

    def chip(step):
        return lax.rem(x + step, nx)

    def peer(step):
        return {"tp": chip(step) * CORES + c}

    def remote(src, dst, send_sem, recv_sem, device):
        return pltpu.make_async_remote_copy(
            src_ref=src, dst_ref=dst, send_sem=send_sem, recv_sem=recv_sem,
            device_id=device, device_id_type=MESH,
        )

    def arrived(dst, recv_sem):
        remote(dst, dst, t_send.at[0], recv_sem, partner).wait_recv()

    own_target = pltpu.make_async_copy(target, tbuf.at[t], local_sem.at[0])
    own_source = [
        pltpu.make_async_copy(
            source.at[pl.ds(part * half, half)], sbuf.at[0, part], local_sem.at[1 + part])
        for part in range(2)
    ]

    def load(kind, level):
        pair = ((w_query, wq), (w_key, wk), (w_value, wv), (w_out, wo))[kind]
        return pltpu.make_async_copy(
            pair[0].at[level], pair[1].at[level], weight_sem.at[kind, level])

    own_target.start()
    for copy in own_source:
        copy.start()
    load(1, 0).start()
    load(2, 0).start()

    barrier = pltpu.get_barrier_semaphore()
    pl.semaphore_signal(barrier, inc=1, device_id=partner, device_id_type=MESH)
    for step in range(1, nx):
        pl.semaphore_signal(barrier, inc=1, device_id=peer(step), device_id_type=MESH)
    for step in range(1, sp):
        pl.semaphore_signal(
            barrier, inc=1, device_id={"sp": lax.rem(s + step, sp)}, device_id_type=MESH)
    pl.semaphore_wait(barrier, 1 + (nx - 1) + (sp - 1))

    sends = []

    drains = []

    def finish():
        for drain in drains:
            drain()
        for copy in sends:
            copy.wait_send()

    def go(copy):
        copy.start()
        sends.append(copy)

    for step in range(1, nx):
        go(remote(target, tbuf.at[t], t_send.at[step], t_recv.at[t], peer(step)))
    go(remote(target, tbuf.at[t], t_send.at[0], t_recv.at[t], partner))
    for part in range(2):
        block = source.at[pl.ds(part * half, half)]
        for piece in range(2):
            span = pl.ds(piece * (half // 2), half // 2)
            for step in range(1, nx):
                unit = 2 * (nx - step) + part
                go(remote(block.at[span], sbuf.at[unit, 0, span], s_send.at[step, 2 * part + piece],
                          s_recv.at[unit, piece], peer(step)))
        go(remote(block, sbuf.at[1, part], s_psend.at[part], s_recv.at[1, part], partner))

    def project(index):
        unit = index // depth
        level = index % depth
        block = sbuf[unit].reshape(rows, width)
        start = pl.multiple_of(unit * rows, rows)
        k = jnp.dot(block, wk[level], preferred_element_type=F32)
        keys[level, pl.ds(start, rows), :] = k.astype(BF16)
        v = jnp.dot(block, wv[level], preferred_element_type=F32)
        values[level, :, pl.ds(start, rows)] = v.T.astype(BF16)

    def query_copy(level, step):
        return remote(qbuf.at[level, s], qbuf.at[level, s], q_send.at[level, step],
                      q_recv.at[level, s], {"sp": lax.rem(s + step, sp)})

    def drain_queries(level):
        for step in range(1, sp):
            query_copy(level, step).wait_send()

    def result_copies(level, j):
        return (
            remote(osend.at[level, j], orecv.at[level, s], o_send.at[level, j],
                   o_recv.at[level, s], {"sp": j}),
            remote(ssend.at[level, j], srecv.at[level, s], e_send.at[level, j],
                   e_recv.at[level, s], {"sp": j}),
        )

    def drain_results(level):
        for step in range(1, sp):
            for copy in result_copies(level, lax.rem(s + step, sp)):
                copy.wait_send()

    def target_relay(step):
        slot = chip(step) * CORES + c
        return remote(tbuf.at[slot], tbuf.at[slot], t_fsend.at[step], t_recv.at[slot], partner)

    def source_relay(unit, piece):
        span = pl.ds(piece * (half // 2), half // 2)
        return remote(sbuf.at[unit, 0, span], sbuf.at[unit, 1, span], s_fsend.at[unit, piece],
                      s_recv.at[unit, 2 + piece], partner)

    def drain_relays():
        for step in range(1, nx):
            target_relay(step).wait_send()
        for unit in range(2, units):
            for piece in range(2):
                source_relay(unit, piece).wait_send()

    def make_queries(level):
        q = jnp.dot(normed[...].reshape(tp * trows, width), wq[level], preferred_element_type=F32)
        qbuf[level, s] = q.astype(BF16)
        for step in range(1, sp):
            query_copy(level, step).start()

    def first_queries():
        own_target.wait()
        for step in range(1, nx):
            slot = chip(step) * CORES + c
            arrived(tbuf.at[slot], t_recv.at[slot])
            target_relay(step).start()
        for step in range(nx):
            slot = chip(step) * CORES + partner_c
            arrived(tbuf.at[slot], t_recv.at[slot])

        @pl.loop(0, tp)
        def _(block):
            value = tbuf[block].astype(F32)
            stream[block] = value
            normed[block] = normalize(value, gains[0, 0:1, :]).astype(BF16)

        load(0, 0).wait()
        make_queries(0)

    @pl.loop(0, units * depth - (depth - 1))
    def _(index):
        unit = index // depth
        level = index % depth

        @pl.when(index == 0)
        def _():
            for copy in own_source:
                copy.wait()
            load(1, 0).wait()
            load(2, 0).wait()
            load(0, 0).start()
            for later in range(1, depth):
                load(1, later).start()
                load(2, later).start()
            load(3, 0).start()
            for later in range(1, depth):
                load(0, later).start()
                load(3, later).start()

        for later in range(1, depth):
            @pl.when(index == later)
            def _():
                load(1, later).wait()
                load(2, later).wait()

        @pl.when(index == depth)
        def _():
            first_queries()
            for part in range(2):
                arrived(sbuf.at[1, part], s_recv.at[1, part])

        @pl.when(jnp.logical_and(unit >= 2, level == 0))
        def _():
            for piece in range(2):
                span = pl.ds(piece * (half // 2), half // 2)
                arrived(sbuf.at[unit, 0, span], s_recv.at[unit, piece])
                source_relay(unit, piece).start()
            for piece in range(2):
                span = pl.ds(piece * (half // 2), half // 2)
                arrived(sbuf.at[unit, 1, span], s_recv.at[unit, 2 + piece])

        project(index)

    drains += [drain_relays, functools.partial(drain_queries, 0)]

    both = jnp.minimum(s, sp - 1 - s)

    def near(i):
        side = jnp.where(i % 2 == 1, s - (i + 1) // 2, s + i // 2)
        rest = jnp.where(s < sp - 1 - s, i, sp - 1 - i)
        return jnp.where(i <= 2 * both, side, rest)

    for layer in range(depth):
        last = layer == depth - 1

        @pl.loop(0, sp)
        def _(i):
            j = near(sp - 1 - i if layer == 0 else i)

            @pl.when(j != s)
            def _():
                arrived(qbuf.at[layer, j], q_recv.at[layer, j])

            q = qbuf[layer, j]
            peaks, totals = [], []
            for h in range(heads):
                cols = slice(h * HEAD, (h + 1) * HEAD)
                scores = lax.dot_general(
                    keys[layer, :, cols], q[:, cols], (((1,), (1,)), ((), ())),
                    preferred_element_type=F32)
                peak = jnp.max(scores, axis=0, keepdims=True) * score_scale
                weights = jnp.exp2(scores * score_scale - peak)
                totals.append(jnp.sum(weights, axis=0, keepdims=True))
                peaks.append(peak)
                o = jnp.dot(values[layer, cols, :], weights.astype(BF16), preferred_element_type=F32)
                osend[layer, j, cols, :] = o.astype(BF16)
            ssend[layer, j] = jnp.concatenate(peaks + totals, axis=0)

            @pl.when(j != s)
            def _():
                for copy in result_copies(layer, j):
                    copy.start()

            @pl.when(j == s)
            def _():
                orecv[layer, s] = osend[layer, s]
                srecv[layer, s] = ssend[layer, s]

        drains.append(functools.partial(drain_results, layer))
        if layer == 0:
            @pl.loop(units * depth - (depth - 1), units * depth)
            def _(index):
                project(index)
        load(3, layer).wait()

        for step in range(1, sp):
            j = lax.rem(s + step, sp)
            arrived(orecv.at[layer, j], o_recv.at[layer, j])
            arrived(srecv.at[layer, j], e_recv.at[layer, j])
        peaks = [srecv[layer, j, 0:heads, :] for j in range(sp)]
        top = functools.reduce(jnp.maximum, peaks)
        share = [jnp.exp2(p - top) for p in peaks]
        total = sum(share[j] * srecv[layer, j, heads:2 * heads, :] for j in range(sp))
        share = [one / total for one in share]
        for h in range(heads):
            cols = slice(h * HEAD, (h + 1) * HEAD)
            mixed = sum(share[j][h:h + 1, :] * orecv[layer, j, cols, :].astype(F32) for j in range(sp))
            attended[:, cols] = mixed.T.astype(BF16)

        tile = min(512, width)
        for n in range(width // tile):
            cols = slice(n * tile, (n + 1) * tile)
            part = jnp.dot(attended[...], wo[layer, :, cols], preferred_element_type=F32)
            pbuf[layer, :, :, :, cols] = part.astype(BF16).reshape(nx, CORES, trows, tile)

        order = [chip(step) for step in list(range(1, nx)) + [0]]
        for b in order:
            go(remote(pbuf.at[layer, b, partner_c], half_in.at[layer, b], h_send.at[layer, b],
                      h_recv.at[layer, b], partner))
        if not last:
            for k, b in enumerate(order):
                arrived(half_in.at[layer, b], h_recv.at[layer, b])
                both_cores = pbuf[layer, b, c].astype(F32) + half_in[layer, b].astype(F32)
                chip_sum[layer, x, c, b] = both_cores.astype(BF16)
                own = chip_sum.at[layer, x, c, b]
                for step in range(1, nx):
                    go(remote(own, own, c_send.at[layer, step, k], c_recv.at[layer, x, b], peer(step)))
                go(remote(own, own, c_psend.at[layer, k], c_frecv.at[layer, x, b], partner))
            for step in range(1, nx):
                a = chip(step)
                for k in range(nx):
                    b = lax.rem(a + 1 + k, nx)
                    other = chip_sum.at[layer, a, c, b]
                    arrived(other, c_recv.at[layer, a, b])
                    go(remote(other, other, c_fsend.at[layer, step, k], c_frecv.at[layer, a, b], partner))
            for step in range(nx):
                a = chip(step)
                for k in range(nx):
                    b = lax.rem(a + 1 + k, nx)
                    arrived(chip_sum.at[layer, a, partner_c, b], c_frecv.at[layer, a, b])
            load(0, layer + 1).wait()

            @pl.loop(0, tp)
            def _(block):
                projected = sum(
                    chip_sum[layer, a, block % CORES, block // CORES].astype(F32) for a in range(nx))
                value = stream[block] + normalize(projected, gains[layer, 1:2, :])
                stream[block] = value
                normed[block] = normalize(value, gains[layer + 1, 0:1, :]).astype(BF16)

            make_queries(layer + 1)
            drains.append(functools.partial(drain_queries, layer + 1))
        else:
            for step in range(1, nx):
                b = chip(step)
                arrived(half_in.at[layer, b], h_recv.at[layer, b])
                both_cores = pbuf[layer, b, c].astype(F32) + half_in[layer, b].astype(F32)
                fin[0, b] = both_cores.astype(BF16)
                go(remote(fin.at[0, b], fin.at[1, x], f_send.at[step], f_recv.at[x], peer(step)))
            arrived(half_in.at[layer, x], h_recv.at[layer, x])
            projected = pbuf[layer, x, c].astype(F32) + half_in[layer, x].astype(F32)
            for step in range(1, nx):
                b = chip(step)
                arrived(fin.at[1, b], f_recv.at[b])
                projected = projected + fin[1, b].astype(F32)
            value = stream[t] + normalize(projected, gains[layer, 1:2, :])
            out[...] = value.astype(out.dtype)

    finish()


def fused_body(nx, sp, target, source, w_query, w_key, w_value, w_out, gains):
    depth, width, local_width = w_query.shape
    trows, rows = target.shape[0], source.shape[0]
    tp = nx * CORES
    block_rows = tp * trows
    heads = local_width // HEAD
    units = 2 * nx
    vmem = pltpu.VMEM
    dma = pltpu.SemaphoreType.DMA
    anywhere = pl.BlockSpec(memory_space=pl.ANY)
    whole = pl.BlockSpec(memory_space=pltpu.VMEM)
    return pl.pallas_call(
        functools.partial(fused_kernel, nx, sp, depth),
        out_shape=jax.ShapeDtypeStruct((trows, width), BF16),
        in_specs=[anywhere] * 6 + [whole],
        out_specs=whole,
        scratch_shapes=[
            vmem((tp, trows, width), BF16),
            vmem((units, 2, rows // 2, width), BF16),
            vmem(w_query.shape, BF16),
            vmem(w_key.shape, BF16),
            vmem(w_value.shape, BF16),
            vmem(w_out.shape, BF16),
            vmem((depth, units * rows, local_width), BF16),
            vmem((depth, local_width, units * rows), BF16),
            vmem((tp, trows, width), F32),
            vmem((tp, trows, width), BF16),
            vmem((depth, sp, block_rows, local_width), BF16),
            vmem((depth, sp, local_width, block_rows), BF16),
            vmem((depth, sp, local_width, block_rows), BF16),
            vmem((depth, sp, 2 * heads, block_rows), F32),
            vmem((depth, sp, 2 * heads, block_rows), F32),
            vmem((block_rows, local_width), BF16),
            vmem((depth, nx, CORES, trows, width), BF16),
            vmem((depth, nx, trows, width), BF16),
            vmem((depth, nx, CORES, nx, trows, width), BF16),
            vmem((2, nx, trows, width), BF16),
            dma((3,)), dma((4, depth)),
            dma((nx,)), dma((tp,)), dma((nx,)),
            dma((2,)), dma((nx, 4)), dma((units, 4)), dma((units, 2)),
            dma((depth, sp)), dma((depth, sp)),
            dma((depth, sp)), dma((depth, sp)), dma((depth, sp)), dma((depth, sp)),
            dma((depth, nx)), dma((depth, nx)),
            dma((depth, nx, nx)), dma((depth, nx)), dma((depth, nx, nx)),
            dma((depth, nx, nx)), dma((depth, nx, nx)),
            dma((nx,)), dma((nx,)),
        ],
        compiler_params=pltpu.CompilerParams(
            collective_id=0, has_side_effects=True, vmem_limit_bytes=60 * 1024 * 1024),
    )(target, source, w_query, w_key, w_value, w_out, gains)


def split_heads(row_block):
    return row_block.reshape(row_block.shape[0], row_block.shape[1] // HEAD, HEAD)


def body(target, source, w_query, w_key, w_value, w_out, gains):
    local_width = w_query.shape[2]
    score_scale = HEAD ** (-0.5)
    depth = w_query.shape[0]
    project_shard_part = lax.all_gather(source, "tp", axis=0, tiled=True)
    layer_parts = [
        jnp.stack(
            [
                jnp.dot(project_shard_part, w_key[level], preferred_element_type=jnp.float32),
                jnp.dot(project_shard_part, w_value[level], preferred_element_type=jnp.float32),
            ]
        )
        for level in range(depth)
    ]
    projected_source = jnp.stack(layer_parts).astype(jnp.bfloat16)
    stream = target.astype(jnp.float32)
    for layer_index in range(depth):
        normed = normalize(stream, gains[layer_index, 0]).astype(jnp.bfloat16)
        query_weight = w_query[layer_index]
        queries = jnp.dot(
            lax.all_gather(normed, "tp", axis=0, tiled=True),
            query_weight,
            preferred_element_type=jnp.float32,
        ).astype(jnp.bfloat16)
        row_count = queries.shape[0]
        keys_here = projected_source[layer_index, 0]
        values_here = projected_source[layer_index, 1]
        every_query = lax.all_gather(queries, "sp", axis=0, tiled=True)
        scores = (
            jnp.einsum(
                "qhd,khd->hqk",
                split_heads(every_query),
                split_heads(keys_here),
                preferred_element_type=jnp.float32,
            )
            * score_scale
        )
        row_peak = lax.pmax(jnp.max(scores, axis=2), "sp")
        weights = jnp.exp(scores - row_peak[:, :, None])
        local_summed = jnp.einsum(
            "hqk,khd->hqd",
            weights.astype(jnp.bfloat16),
            split_heads(values_here),
            preferred_element_type=jnp.float32,
        )
        summed, row_total = (
            lax.psum_scatter(
                local_summed.astype(jnp.bfloat16), "sp", scatter_dimension=1, tiled=True
            ).astype(jnp.float32),
            lax.psum_scatter(
                jnp.sum(weights, axis=2).astype(jnp.bfloat16), "sp", scatter_dimension=1, tiled=True
            ).astype(jnp.float32),
        )
        heads_out = summed / row_total[:, :, None]
        attended = (
            jnp.transpose(heads_out, (1, 0, 2)).reshape(row_count, local_width).astype(jnp.bfloat16)
        )
        out_weight = w_out[layer_index]
        projected = lax.psum_scatter(
            jnp.dot(attended, out_weight, preferred_element_type=jnp.float32).astype(jnp.bfloat16),
            "tp",
            scatter_dimension=0,
            tiled=True,
        ).astype(jnp.float32)
        stream = stream + normalize(projected, gains[layer_index, 1])
    return stream.astype(jnp.bfloat16)


def solution(mesh):
    in_specs = (
        P(("grp", "sp", "tp"), None),
        P(("grp", "sp", "tp"), None),
        P(None, None, "tp"),
        P(None, None, "tp"),
        P(None, None, "tp"),
        P(None, "tp", None),
        P(),
    )
    out_specs = P(("grp", "sp", "tp"), None)
    sp, tp = mesh.shape["sp"], mesh.shape["tp"]

    def run(target, source, w_query, w_key, w_value, w_out, gains):
        trows, rows, local_width = target.shape[0], source.shape[0], w_query.shape[2]
        tiles = (trows % 16 == 0 and (tp * trows) % 128 == 0 and rows % 128 == 0 and rows % 64 == 0
                 and local_width % (4 * HEAD) == 0 and tp % CORES == 0)
        form = functools.partial(fused_body, tp // CORES, sp) if tiles else body
        return form(target, source, w_query, w_key, w_value, w_out, gains)

    return jax.shard_map(run, mesh=mesh, in_specs=in_specs, out_specs=out_specs, check_vma=False)
```
